32 devices in a mesh: sp: 16 (over z, y, x), tp: 2 (over core).
Axes of the slice: x: 2, y: 2, z: 4, core: 2. Of those that a mesh axis runs over, the one named last changes fastest.
Arguments:
- activations: bfloat16 [16384, 2048], P(('sp', 'tp')), may hold values from -6 to 6
- input_norm_scale: float32 [2048], replicated, may hold values from 0.1 to 1.9
- value_weight_matrix: bfloat16 [2048, 1024], P(None, 'tp'), may hold values from -0.125 to 0.125
- gate_weight_matrix: bfloat16 [2048, 1024], P(None, 'tp'), may hold values from -0.125 to 0.125
- write_weight_matrix: bfloat16 [2048, 1024], P(None, 'tp'), may hold values from -0.125 to 0.125
- read_weight_matrix: bfloat16 [2048, 1024], P(None, 'tp'), may hold values from -0.125 to 0.125
- step_weight_matrix: bfloat16 [2048, 16], replicated, may hold values from -0.125 to 0.125
- pooling_input_matrix: bfloat16 [2048, 1024], P(None, 'tp'), may hold values from -0.125 to 0.125
- value_filter_weight: float32 [4, 1024], P(None, 'tp'), may hold values from -3 to 3
- write_filter_weight: float32 [4, 1024], P(None, 'tp'), may hold values from -3 to 3
- read_filter_weight: float32 [4, 1024], P(None, 'tp'), may hold values from -3 to 3
- head_log_decay_rate: float32 [16], replicated, may hold values from -12 to 0, as said below
- step_bias_offset: float32 [16, 16384], P('tp', 'sp'), may hold values from -3 to 0, as said below
- position_log_decay: float32 [16, 16384], P('tp', 'sp'), may hold values from -2 to 0, as said below
- gated_norm_scale: float32 [1024], P('tp'), may hold values from 0.1 to 1.9
- pooling_group_matrix: bfloat16 [16, 64, 64], P('tp'), may hold values from -0.75 to 0.75
- pooling_channel_scale: float32 [1024], P('tp'), may hold values from 0.1 to 1.9
- state_output_matrix: bfloat16 [1024, 2048], P('tp'), may hold values from -0.125 to 0.125
- pooling_output_matrix: bfloat16 [1024, 2048], P('tp'), may hold values from -0.125 to 0.125
Outputs:
- mixed: bfloat16 [16384, 2048], P(('sp', 'tp'))
The draws below stay inside these ranges and needn't reach their ends.
Inputs may be any that keep to these rules, and one draw needn't show every extreme that they name: `head_log_decay_rate`: each head's logarithmic decay rate. `step_bias_offset`: constant over each block of 128 positions. `position_log_decay`: zero except at a few positions of the sequence.
All inputs are finite; a program needn't handle non-finite values.
Results may differ from the reference program's by a relative error of at most 0.017.
Values may be sent and summed in bfloat16 or wider, within the bound.
A program may use at most 128 MiB of HBM per device.

```python
import jax
import jax.numpy as jnp
from jax import lax

D = 2048
HEADS = 16
HEAD_DIM = 64
GROUPS = 8
STATE = 128
CONV = 4
BLOCK = 128
POOL_GROUPS = 16
POOL_DIM = 64
TOKENS = 16384
N_TP = 2


def draw_head_log_decay_rate(key, part):
    ranking = jax.random.permutation(key, HEADS)
    slow_count = HEADS // 2
    spread = jax.random.uniform(jax.random.fold_in(key, 1), (HEADS,), jnp.float32)
    slow_log = jnp.log(1.0 / TOKENS) + spread * jnp.log(6.0)
    fast_log = jnp.log(0.06) + spread * (jnp.log(0.4) - jnp.log(0.06))
    return jnp.where(ranking < slow_count, slow_log, fast_log).astype(jnp.float32)


def draw_step_bias_offset(key, part):
    lowest = -3.0
    highest = -1.0
    levels = jax.random.uniform(key, (HEADS, TOKENS // BLOCK), jnp.float32, lowest, highest)
    return jnp.repeat(levels, BLOCK, axis=1)


def draw_position_log_decay(key, part):
    places = jax.random.randint(key, (4,), 0, TOKENS)
    depth = jnp.log(jax.random.uniform(jax.random.fold_in(key, 1), (HEADS, 4), jnp.float32, 0.5, 0.8))
    hits = (jnp.arange(TOKENS)[None, :] == places[:, None]).astype(jnp.float32)
    return jnp.dot(depth, hits, precision=lax.Precision.HIGHEST)


def level_of(rng, shape, pieces, least, largest):
    def one(axis_at, parts):
        heights = jax.random.uniform(jax.random.fold_in(jax.random.fold_in(rng, 6), axis_at), (parts,), jnp.float32, least / len(pieces), largest / len(pieces))
        return jnp.repeat(jnp.exp(heights), shape[axis_at] // parts).reshape((-1,) + (1,) * (len(shape) - axis_at - 1))

    gain = one(*pieces[0])
    for cut in pieces[1:]:
        gain = gain * one(*cut)
    return gain


def gaussian(stream_key, extent, width, most, pieces=(), held_as=jnp.bfloat16):
    result = width * jax.random.normal(stream_key, extent, jnp.float32)
    if pieces:
        result = result * level_of(stream_key, extent, pieces, -0.22, 0.18)
    return jnp.clip(result, -most, most).astype(held_as)


def setup_inputs(seed: int = 0) -> dict:
    streams_of = jax.random.split(jax.random.key(seed), 20)
    return {
        "activations": gaussian(streams_of[0], (TOKENS, D), 1.0, 6.0, ((0, 32),)),
        "input_norm_scale": jnp.clip(1.0 + 0.18 * jax.random.normal(streams_of[1], (D,), jnp.float32), 0.1, 1.9),
        "value_weight_matrix": gaussian(streams_of[2], (D, HEADS * HEAD_DIM), D ** -0.5, 0.125, ((1, 2),)),
        "gate_weight_matrix": gaussian(streams_of[3], (D, HEADS * HEAD_DIM), D ** -0.5, 0.125, ((1, 2),)),
        "write_weight_matrix": gaussian(streams_of[4], (D, GROUPS * STATE), D ** -0.5, 0.125, ((1, 2),)),
        "read_weight_matrix": gaussian(streams_of[5], (D, GROUPS * STATE), D ** -0.5, 0.125, ((1, 2),)),
        "step_weight_matrix": gaussian(streams_of[6], (D, HEADS), D ** -0.5, 0.125),
        "pooling_input_matrix": gaussian(streams_of[7], (D, POOL_GROUPS * POOL_DIM), D ** -0.5, 0.125, ((1, 2),)),
        "value_filter_weight": gaussian(streams_of[8], (CONV, HEADS * HEAD_DIM), CONV ** -0.5, 3.0, ((1, 2),), jnp.float32),
        "write_filter_weight": gaussian(streams_of[9], (CONV, GROUPS * STATE), CONV ** -0.5, 3.0, ((1, 2),), jnp.float32),
        "read_filter_weight": gaussian(streams_of[10], (CONV, GROUPS * STATE), CONV ** -0.5, 3.0, ((1, 2),), jnp.float32),
        "head_log_decay_rate": draw_head_log_decay_rate(jax.random.fold_in(streams_of[19], 71), 0),
        "step_bias_offset": draw_step_bias_offset(jax.random.fold_in(streams_of[19], 71), 0),
        "position_log_decay": draw_position_log_decay(jax.random.fold_in(streams_of[19], 71), 0),
        "gated_norm_scale": jnp.clip(1.0 + 0.18 * jax.random.normal(streams_of[14], (HEADS * HEAD_DIM,), jnp.float32), 0.1, 1.9),
        "pooling_group_matrix": gaussian(streams_of[15], (POOL_GROUPS, POOL_DIM, POOL_DIM), POOL_DIM ** -0.5, 0.75, ((0, 2),)),
        "pooling_channel_scale": jnp.clip(1.0 + 0.18 * jax.random.normal(streams_of[16], (POOL_GROUPS * POOL_DIM,), jnp.float32), 0.1, 1.9),
        "state_output_matrix": gaussian(streams_of[17], (HEADS * HEAD_DIM, D), (HEADS * HEAD_DIM + POOL_GROUPS * POOL_DIM) ** -0.5, 0.125, ((0, 2),)),
        "pooling_output_matrix": gaussian(streams_of[18], (POOL_GROUPS * POOL_DIM, D), (HEADS * HEAD_DIM + POOL_GROUPS * POOL_DIM) ** -0.5, 0.125, ((0, 2),)),
    }


EPS = 1e-06

def rounded(value):
    return lax.optimization_barrier(value.astype(jnp.bfloat16)).astype(jnp.float32)

def convolve(signal, taps):
    length = signal.shape[0]
    padded = jnp.pad(signal.astype(jnp.float32), ((taps.shape[0] - 1, 0), (0, 0)))
    summed = jnp.zeros(signal.shape, jnp.float32)
    for offset in range(taps.shape[0]):
        summed = summed + taps[offset] * padded[offset:offset + length]
    return jax.nn.silu(summed).astype(jnp.bfloat16)

def reference(activations, input_norm_scale, value_weight_matrix, gate_weight_matrix, write_weight_matrix, read_weight_matrix, step_weight_matrix, pooling_input_matrix, value_filter_weight, write_filter_weight, read_filter_weight, head_log_decay_rate, step_bias_offset, position_log_decay, gated_norm_scale, pooling_group_matrix, pooling_channel_scale, state_output_matrix, pooling_output_matrix):
    inputs_wide = activations.astype(jnp.float32)
    normed = (inputs_wide * lax.rsqrt(lax.optimization_barrier(jnp.mean(inputs_wide * inputs_wide, axis=-1, keepdims=True)) + EPS) * input_norm_scale).astype(jnp.bfloat16)
    value_in, gate_in, write_in, read_in, step_in, pool_in = [jnp.dot(normed, matrix, preferred_element_type=jnp.float32).astype(jnp.bfloat16) for matrix in (value_weight_matrix, gate_weight_matrix, write_weight_matrix, read_weight_matrix, step_weight_matrix, pooling_input_matrix)]
    values = convolve(value_in, value_filter_weight)
    writes = convolve(write_in, write_filter_weight)
    reads = convolve(read_in, read_filter_weight)
    step_length_value = jax.nn.softplus(step_in.astype(jnp.float32) + step_bias_offset.T)
    decay_logarithm_value = position_log_decay.T - jnp.exp(head_log_decay_rate) * step_length_value
    blocks = TOKENS // BLOCK
    repeat = HEADS // GROUPS
    values = values.reshape(blocks, BLOCK, HEADS, HEAD_DIM).astype(jnp.float32)
    writes = writes.reshape(blocks, BLOCK, GROUPS, STATE).astype(jnp.float32)
    reads = reads.reshape(blocks, BLOCK, GROUPS, STATE).astype(jnp.float32)
    cumulative = jnp.cumsum(decay_logarithm_value.reshape(blocks, BLOCK, HEADS), axis=1).transpose(0, 2, 1)
    step_heads = step_length_value.reshape(blocks, BLOCK, HEADS).transpose(0, 2, 1)
    causal = jnp.tril(jnp.ones((BLOCK, BLOCK), bool))
    affinity = jnp.repeat(jnp.einsum('btgn,bsgn->bgts', reads, writes), repeat, axis=1)
    spacing = cumulative[:, :, :, None] - cumulative[:, :, None, :]
    within = rounded(affinity * jnp.exp(jnp.where(causal, spacing, -jnp.inf)) * step_heads[:, :, None, :])
    inside = jnp.einsum('bhts,bshp->bthp', within, values)
    to_end = jnp.exp(cumulative[:, :, -1:] - cumulative) * step_heads
    weighted = rounded(values * to_end.transpose(0, 2, 1)[..., None])
    writes_heads = jnp.repeat(writes, repeat, axis=2)
    contrib = jnp.einsum('bshp,bshn->bhpn', weighted, writes_heads)
    totals = cumulative[:, :, -1]

    def advance(carried, block_pair):
        block_contrib, block_total = block_pair
        return (carried * jnp.exp(block_total)[:, None, None] + block_contrib, carried)
    _, entering = lax.scan(advance, jnp.zeros((HEADS, HEAD_DIM, STATE), jnp.float32), (contrib, totals))
    reads_heads = jnp.repeat(reads, repeat, axis=2)
    carried_in = jnp.einsum('bthn,bhpn->bthp', reads_heads, rounded(entering))
    state_y = inside + carried_in * jnp.exp(cumulative).transpose(0, 2, 1)[..., None]
    gated = state_y.reshape(TOKENS, HEADS * HEAD_DIM) * jax.nn.silu(gate_in.astype(jnp.float32))
    grouped = gated.reshape(TOKENS, GROUPS, repeat * HEAD_DIM)
    grouped = grouped * lax.rsqrt(lax.optimization_barrier(jnp.mean(grouped * grouped, axis=-1, keepdims=True)) + EPS)
    state_branch = (grouped.reshape(TOKENS, HEADS * HEAD_DIM) * gated_norm_scale).astype(jnp.bfloat16)
    pool_width = POOL_GROUPS * POOL_DIM
    pool_wide = pool_in.astype(jnp.float32)
    running = jnp.concatenate([jnp.zeros((1, pool_width), jnp.float32), jnp.cumsum(pool_wide, axis=0)], axis=0)
    level = jnp.arange(pool_width, dtype=jnp.int32) // POOL_DIM % 4
    window_len = jnp.power(2, level + 1).astype(jnp.int32)[None, :]
    position = jnp.arange(TOKENS, dtype=jnp.int32)[:, None]
    lowest = jnp.maximum(position + 1 - window_len, 0).astype(jnp.int32)
    lower_sum = jnp.take_along_axis(running, lowest, axis=0)
    counted = jnp.minimum(position + 1, window_len).astype(jnp.float32)
    pool_diff = rounded((running[1:] - lower_sum) / counted - pool_wide)
    pooled = jnp.einsum('tgc,gcd->tgd', pool_diff.reshape(TOKENS, POOL_GROUPS, POOL_DIM), pooling_group_matrix.astype(jnp.float32))
    pool_branch = (pooled.reshape(TOKENS, pool_width) * pooling_channel_scale).astype(jnp.bfloat16)
    head_cols = HEADS * HEAD_DIM // N_TP
    pool_cols = pool_width // N_TP
    summed = jnp.zeros((TOKENS, D), jnp.float32)
    for member in range(N_TP):
        part_sum = jnp.dot(state_branch[:, member * head_cols:(member + 1) * head_cols], state_output_matrix[member * head_cols:(member + 1) * head_cols], preferred_element_type=jnp.float32) + jnp.dot(pool_branch[:, member * pool_cols:(member + 1) * pool_cols], pooling_output_matrix[member * pool_cols:(member + 1) * pool_cols], preferred_element_type=jnp.float32)
        summed = summed + rounded(part_sum)
    return summed.astype(jnp.bfloat16)
```

```python
import functools

import jax
import jax.numpy as jnp
from jax import lax
from jax.experimental import pallas as pl
from jax.experimental.pallas import tpu as pltpu
from jax.sharding import PartitionSpec as P

HEAD_DIM = 64
STATE = 128
BLOCK = 128
POOL_DIM = 64
TAIL = 16
EPS = 1e-06
F32 = jnp.float32
BF16 = jnp.bfloat16
HIGHEST = lax.Precision.HIGHEST

VMEM = pl.BlockSpec(memory_space=pltpu.VMEM)
ANY = pl.BlockSpec(memory_space=pl.ANY)
PARAMS = pltpu.CompilerParams(vmem_limit_bytes=48 * 1024 * 1024)


def iota(shape, axis):
    return lax.broadcasted_iota(jnp.int32, shape, axis)


def silu(v):
    return v / (1.0 + jnp.exp(-v))


def rows_at(i, n):
    return pl.ds(pl.multiple_of(i * n, n), n)


def tdot(a, b):
    return lax.dot_general(a, b, (((1,), (1,)), ((), ())), preferred_element_type=F32)


def spread(rows, width):
    heads = rows.shape[0]
    pick = (iota((heads, heads * width), 1) // width == iota((heads, heads * width), 0)).astype(F32)
    return lax.dot_general(
        rows, pick, (((0,), (0,)), ((), ())), precision=HIGHEST, preferred_element_type=F32
    )


def norm_rows(x, scale):
    wide = x.astype(F32)
    mean = jnp.mean(wide * wide, axis=-1, keepdims=True)
    return (wide * lax.rsqrt(mean + EPS) * scale).astype(BF16)


def project(xn, i, tile, w):
    part = jnp.dot(xn[pl.ds(pl.multiple_of(TAIL + i * tile, TAIL), tile), :], w[...], preferred_element_type=F32)
    return part.astype(BF16).astype(F32)


def conv_matrix(xn, w, taps, out, ext, length, tile):
    cols = w.shape[1]
    reach = taps.shape[0] - 1
    ext[0:TAIL, 0:cols] = (
        jnp.dot(xn[0:TAIL, :], w[...], preferred_element_type=F32).astype(BF16).astype(F32)
    )

    @pl.loop(0, length // tile)
    def _(i):
        ext[TAIL : TAIL + tile, 0:cols] = project(xn, i, tile, w)
        total = taps[0:1, :] * ext[TAIL - reach : TAIL - reach + tile, 0:cols]
        for k in range(1, reach + 1):
            total = total + taps[k : k + 1, :] * ext[TAIL - reach + k : TAIL - reach + k + tile, 0:cols]
        out[rows_at(i, tile), :] = silu(total).astype(BF16)
        ext[0:TAIL, 0:cols] = ext[tile : tile + TAIL, 0:cols]


def kernel_a(tp, *refs):
    xs, halos = refs[:tp], refs[tp : 2 * tp]
    (scale, wv, ww, ws, tv, tw, rate, bias, extra) = refs[2 * tp : 2 * tp + 9]
    (xn, vals, writes, step_o, cum_o, cumg_o, entry, pack) = refs[2 * tp + 9 : 2 * tp + 17]
    xv, wvb, wwb, ext, steps, carried, sems = refs[2 * tp + 17 :]
    own = xs[0].shape[0]
    length = own * tp
    rank = lax.axis_index("tp")
    copies = [pltpu.make_async_copy(xs[d], xv.at[d], sems.at[d]) for d in range(tp)]
    copies.append(pltpu.make_async_copy(wv, wvb, sems.at[tp]))
    copies.append(pltpu.make_async_copy(ww, wwb, sems.at[tp + 1]))
    for c in copies:
        c.start()
    halo = halos[0][...].astype(F32)
    for h in halos[1:]:
        halo = halo + h[...].astype(F32)
    xn[0:TAIL, :] = norm_rows(halo, scale[...])
    small = min(64, own)
    for d in range(tp):
        copies[d].wait()
        source = lax.rem(rank - d + tp, tp)

        @pl.loop(0, own // small)
        def _(i):
            at = pl.multiple_of(TAIL + source * own + i * small, TAIL)
            xn[pl.ds(at, small), :] = norm_rows(xv[d, rows_at(i, small), :], scale[...])

    tile = min(256, length)
    heads = bias.shape[0]

    @pl.loop(0, length // tile)
    def _(i):
        s = project(xn, i, tile, ws)
        for b in range(tile // BLOCK):
            steps[i * (tile // BLOCK) + b] = s[b * BLOCK : (b + 1) * BLOCK, :].T

    copies[tp].wait()
    conv_matrix(xn, wvb, tv, vals, ext, length, tile)
    copies[tp + 1].wait()
    conv_matrix(xn, wwb, tw, writes, ext, length, tile)

    blocks = length // BLOCK
    upper = (iota((BLOCK, BLOCK), 0) <= iota((BLOCK, BLOCK), 1)).astype(F32)
    all_rates = jnp.exp(rate[...])
    own_rate = jnp.zeros((heads, 1), F32)
    for t in range(tp):
        own_rate = own_rate + jnp.where(rank == t, all_rates[t * heads : (t + 1) * heads, :], 0.0)
    carried[...] = jnp.zeros_like(carried)
    groups = ww.shape[1] // STATE
    total = jnp.zeros((heads, BLOCK), F32)
    for k in range(blocks):
        cols = slice(k * BLOCK, (k + 1) * BLOCK)
        every = steps[k]
        mine = jnp.zeros((heads, BLOCK), F32)
        for t in range(tp):
            mine = mine + jnp.where(rank == t, every[t * heads : (t + 1) * heads, :], 0.0)
        pre = mine + bias[:, cols]
        step = jnp.maximum(pre, 0.0) + jnp.log1p(jnp.exp(-jnp.abs(pre)))
        decay = extra[:, cols] - own_rate * step
        cum = jnp.dot(decay, upper, precision=HIGHEST, preferred_element_type=F32)
        step_o[k] = step
        cum_o[k] = cum
        cumg_o[k] = cum + total
        last = jnp.broadcast_to(cum[:, BLOCK - 1 : BLOCK], (heads, BLOCK))
        weight = spread(jnp.exp(last - cum) * step, HEAD_DIM)
        weighted = (vals[cols, :].astype(F32) * weight).astype(BF16)
        grow = jnp.exp(last)
        total = total + last
        for g in range(groups):
            lanes = slice(g * STATE, (g + 1) * STATE)
            contrib = lax.dot_general(
                weighted[:, lanes],
                writes[cols, lanes],
                (((0,), (0,)), ((), ())),
                preferred_element_type=F32,
            )
            entry[k, lanes, :] = carried[lanes, :].astype(BF16)
            repeat = STATE // HEAD_DIM
            for j in range(repeat):
                h = g * repeat + j
                at = slice(h * HEAD_DIM, (h + 1) * HEAD_DIM)
                carried[at, :] = (
                    carried[at, :] * grow[h : h + 1, :] + contrib[j * HEAD_DIM : (j + 1) * HEAD_DIM, :]
                )
    write_pack(pack, carried[...], total)


def write_pack(pack, state, total):
    wide = state.shape[0]
    heads = total.shape[0]
    pack[0:wide, :] = state.astype(BF16)
    high = total.astype(BF16).astype(F32)
    mid = (total - high).astype(BF16).astype(F32)
    low = total - high - mid
    filler = jnp.zeros((pack.shape[0] - wide - 3 * heads, STATE), F32)
    pack[wide:, :] = jnp.concatenate([high, mid, low, filler], axis=0).astype(BF16)


def kernel_scan(heads, *refs):
    packs, out = refs[:-1], refs[-1]
    wide = heads * HEAD_DIM
    passed = jnp.zeros((heads, STATE), F32)
    state = jnp.zeros((wide, STATE), F32)
    for p in packs:
        factor = jnp.exp(passed)
        tall = jnp.concatenate(
            [jnp.broadcast_to(factor[h : h + 1, :], (HEAD_DIM, STATE)) for h in range(heads)], axis=0
        )
        state = state + p[0:wide, :].astype(F32) * tall
        rest = p[wide:, :].astype(F32)
        passed = passed + (
            rest[0:heads, :] + rest[heads : 2 * heads, :] + rest[2 * heads : 3 * heads, :]
        )
    write_pack(out, state, passed)


def kernel_b1(tp, xn_h, wr_h, wg_h, wp_h, tr, pgm, pscale, reads, gate, branch, xn, wr, wg, wp, ext, a2, a4, a8, a16, sems):
    rank = lax.axis_index("tp")
    position0 = lax.axis_index("sp")
    copies = [
        pltpu.make_async_copy(src, dst, sems.at[i])
        for i, (src, dst) in enumerate(((xn_h, xn), (wr_h, wr), (wg_h, wg), (wp_h, wp)))
    ]
    for c in copies:
        c.start()
    copies[0].wait()
    copies[1].wait()
    length = xn.shape[0] - TAIL
    tile = min(256, length)
    conv_matrix(xn, wr, tr, reads, ext, length, tile)
    copies[2].wait()

    @pl.loop(0, length // tile)
    def _(i):
        gate[rows_at(i, tile), :] = jnp.dot(
            xn[pl.ds(pl.multiple_of(TAIL + i * tile, TAIL), tile), :], wg[...], preferred_element_type=F32
        ).astype(BF16)

    copies[3].wait()
    cols = wp.shape[1]
    groups = cols // POOL_DIM
    ext[0:TAIL, 0:cols] = (
        jnp.dot(xn[0:TAIL, :], wp[...], preferred_element_type=F32).astype(BF16).astype(F32)
    )
    level = lax.rem(rank * groups + iota((1, cols), 1) // POOL_DIM, 4)
    window = jnp.where(level == 0, 2, jnp.where(level == 1, 4, jnp.where(level == 2, 8, 16)))
    n = tile + TAIL
    twice = (iota((POOL_DIM, 2 * POOL_DIM), 1) % POOL_DIM == iota((POOL_DIM, 2 * POOL_DIM), 0)).astype(BF16)
    pair = 2 * POOL_DIM
    same = iota((pair, pair), 0) // POOL_DIM == iota((pair, pair), 1) // POOL_DIM

    @pl.loop(0, length // tile)
    def _(i):
        p = project(xn, i, tile, wp)
        ext[TAIL:n, 0:cols] = p
        a2[0:n, :] = ext[0:n, 0:cols] + ext[1 : n + 1, 0:cols]
        a4[0:n, :] = a2[0:n, :] + a2[2 : n + 2, :]
        a8[0:n, :] = a4[0:n, :] + a4[4 : n + 4, :]
        a16[0:n, :] = a8[0:n, :] + a8[8 : n + 8, :]
        total = jnp.where(
            level == 0,
            a2[15 : 15 + tile, :],
            jnp.where(
                level == 1,
                a4[13 : 13 + tile, :],
                jnp.where(level == 2, a8[9 : 9 + tile, :], a16[1 : 1 + tile, :]),
            ),
        )
        at = position0 * length + i * tile + iota((tile, cols), 0)
        counted = jnp.minimum(at + 1, window).astype(F32)
        diff = (total / counted - p).astype(BF16)
        for j in range(groups // 2):
            lanes = slice(j * pair, (j + 1) * pair)
            both = jnp.dot(pgm[lanes, :], twice, preferred_element_type=F32)
            block = jnp.where(same, both, 0.0).astype(BF16)
            mapped = jnp.dot(diff[:, lanes], block, preferred_element_type=F32)
            branch[rows_at(i, tile), lanes] = (mapped * pscale[:, lanes]).astype(BF16)
        ext[0:TAIL, 0:cols] = ext[tile : tile + TAIL, 0:cols]


def kernel_b2(reads, writes, vals, step_i, cum_i, entry, y):
    groups = writes.shape[1] // STATE
    repeat = STATE // HEAD_DIM
    step = step_i[0]
    cum = cum_i[0]
    tall = spread(cum, BLOCK)
    grown = jnp.exp(spread(cum, HEAD_DIM))
    causal = iota((BLOCK, BLOCK), 0) >= iota((BLOCK, BLOCK), 1)
    lane = iota((BLOCK, STATE), 1) // HEAD_DIM
    for g in range(groups):
        lanes = slice(g * STATE, (g + 1) * STATE)
        read = reads[:, lanes]
        affinity = tdot(read, writes[:, lanes])
        value = vals[:, lanes].astype(F32)
        total = tdot(read, entry[0, lanes, :]) * grown[:, lanes]
        for j in range(repeat):
            h = g * repeat + j
            gap = tall[:, h * BLOCK : (h + 1) * BLOCK] - cum[h : h + 1, :]
            within = (
                affinity * jnp.exp(jnp.where(causal, gap, -jnp.inf)) * step[h : h + 1, :]
            ).astype(BF16)
            part = jnp.where(lane == j, value, 0.0).astype(BF16)
            total = total + jnp.dot(within, part, preferred_element_type=F32)
        y[:, lanes] = total


def kernel_c(off, y, reads, gate, branch, cumg, incoming, gnorm, so, po, out):
    groups = y.shape[1] // STATE
    grown = jnp.concatenate([jnp.exp(spread(cumg[b], HEAD_DIM)) for b in range(cumg.shape[0])], axis=0)
    pieces = []
    for g in range(groups):
        lanes = slice(g * STATE, (g + 1) * STATE)
        total = y[:, lanes] + grown[:, lanes] * tdot(reads[:, lanes], incoming[lanes, :])
        gated = total * silu(gate[:, lanes].astype(F32))
        mean = jnp.mean(gated * gated, axis=-1, keepdims=True)
        pieces.append((gated * lax.rsqrt(mean + EPS) * gnorm[:, lanes]).astype(BF16))
    branch_s = jnp.concatenate(pieces, axis=1)
    out[...] = (
        jnp.dot(branch_s, so[...], preferred_element_type=F32)
        + jnp.dot(branch[...], po[...], preferred_element_type=F32)
    ).astype(BF16)


def shape(s, t):
    return jax.ShapeDtypeStruct(s, t)


def cost(flops, size):
    return pl.CostEstimate(flops=int(flops), bytes_accessed=int(size), transcendentals=0)


def shards(
    tp,
    sp,
    activations,
    input_norm_scale,
    value_weight_matrix,
    gate_weight_matrix,
    write_weight_matrix,
    read_weight_matrix,
    step_weight_matrix,
    pooling_input_matrix,
    value_filter_weight,
    write_filter_weight,
    read_filter_weight,
    head_log_decay_rate,
    step_bias_offset,
    position_log_decay,
    gated_norm_scale,
    pooling_group_matrix,
    pooling_channel_scale,
    state_output_matrix,
    pooling_output_matrix,
):
    own, width = activations.shape
    length = own * tp
    vc = value_weight_matrix.shape[1]
    wc = write_weight_matrix.shape[1]
    gc = gate_weight_matrix.shape[1]
    pc = pooling_input_matrix.shape[1]
    heads = vc // HEAD_DIM
    blocks = length // BLOCK
    every = step_weight_matrix.shape[1]
    tile = min(256, length)
    rank = lax.axis_index("tp")

    tail = activations[own - TAIL :, :]
    xs = [activations]
    for d in range(1, tp):
        xs.append(lax.ppermute(activations, "tp", [(i, (i + d) % tp) for i in range(tp)]))
    halos = [
        lax.ppermute(tail, ("sp", "tp"), [(s * tp - 1, s * tp + t) for s in range(1, sp)])
        for t in range(tp)
    ]
    pack_rows = -(-(vc + 3 * heads) // 16) * 16
    xn, vals, writes, step, cum, cumg, entry, pack = pl.pallas_call(
        functools.partial(kernel_a, tp),
        name="front",
        out_shape=(
            shape((TAIL + length, width), BF16),
            shape((length, vc), BF16),
            shape((length, wc), BF16),
            shape((blocks, heads, BLOCK), F32),
            shape((blocks, heads, BLOCK), F32),
            shape((blocks, heads, BLOCK), F32),
            shape((blocks, vc, STATE), BF16),
            shape((pack_rows, STATE), BF16),
        ),
        in_specs=[ANY] * tp + [VMEM] * tp + [VMEM, ANY, ANY] + [VMEM] * 6,
        out_specs=[VMEM] * 8,
        scratch_shapes=[
            pltpu.VMEM((tp, own, width), BF16),
            pltpu.VMEM((width, vc), BF16),
            pltpu.VMEM((width, wc), BF16),
            pltpu.VMEM((TAIL + tile, max(vc, wc)), F32),
            pltpu.VMEM((blocks, every, BLOCK), F32),
            pltpu.VMEM((vc, STATE), F32),
            pltpu.SemaphoreType.DMA((tp + 2,)),
        ],
        compiler_params=PARAMS,
        cost_estimate=cost(2 * length * width * (vc + wc), 4 * width * (length + vc)),
    )(
        *xs,
        *halos,
        input_norm_scale[None, :],
        value_weight_matrix,
        write_weight_matrix,
        step_weight_matrix,
        value_filter_weight,
        write_filter_weight,
        head_log_decay_rate[:, None],
        step_bias_offset,
        position_log_decay,
    )

    def from_before(block, distance):
        return lax.ppermute(block, "sp", [(s - distance, s) for s in range(distance, sp)])

    def combine(packs):
        return pl.pallas_call(
            functools.partial(kernel_scan, heads),
            name="scan",
            out_shape=shape((pack_rows, STATE), BF16),
            in_specs=[VMEM] * len(packs),
            out_specs=VMEM,
            cost_estimate=cost(vc * STATE * 8, vc * STATE * 8),
        )(*packs)

    first = [from_before(pack, d) for d in range(1, 5) if d < sp]

    tall = tile + TAIL + 16
    reads, gate, branch = pl.pallas_call(
        functools.partial(kernel_b1, tp),
        name="middle",
        out_shape=(shape((length, wc), BF16), shape((length, gc), BF16), shape((length, pc), BF16)),
        in_specs=[ANY] * 4 + [VMEM] * 3,
        out_specs=[VMEM] * 3,
        scratch_shapes=[
            pltpu.VMEM((TAIL + length, width), BF16),
            pltpu.VMEM((width, wc), BF16),
            pltpu.VMEM((width, gc), BF16),
            pltpu.VMEM((width, pc), BF16),
            pltpu.VMEM((tall, max(wc, pc)), F32),
            pltpu.VMEM((tall, pc), F32),
            pltpu.VMEM((tall, pc), F32),
            pltpu.VMEM((tall, pc), F32),
            pltpu.VMEM((tall, pc), F32),
            pltpu.SemaphoreType.DMA((4,)),
        ],
        compiler_params=PARAMS,
        cost_estimate=cost(2 * length * width * (gc + wc + pc), 4 * width * (length + vc)),
    )(
        xn,
        read_weight_matrix,
        gate_weight_matrix,
        pooling_input_matrix,
        read_filter_weight,
        pooling_group_matrix.reshape(pc, POOL_DIM),
        pooling_channel_scale[None, :],
    )

    covered = combine(first)
    reach = 4
    second = []
    while reach < sp:
        parts = [covered] + [from_before(covered, d * reach) for d in range(1, 4) if d * reach < sp]
        second.append(parts)
        covered = combine(parts)
        reach *= 4
    incoming = covered

    row = lambda k: (k, 0)
    deep = lambda k: (k, 0, 0)
    y = pl.pallas_call(
        kernel_b2,
        name="inside",
        grid=(blocks,),
        out_shape=shape((length, vc), F32),
        in_specs=[
            pl.BlockSpec((BLOCK, wc), row),
            pl.BlockSpec((BLOCK, wc), row),
            pl.BlockSpec((BLOCK, vc), row),
            pl.BlockSpec((1, heads, BLOCK), deep),
            pl.BlockSpec((1, heads, BLOCK), deep),
            pl.BlockSpec((1, vc, STATE), deep),
        ],
        out_specs=pl.BlockSpec((BLOCK, vc), row),
        cost_estimate=cost(8e9, 8 * length * vc),
    )(reads, writes, vals, step, cum, entry)

    part_tile = min(256, own)
    steps = own // part_tile
    fixed = lambda i, off: (0, 0)
    moving = lambda i, off: (off[0] + i, 0)

    def part(member):
        return pl.pallas_call(
            kernel_c,
            name="back",
            out_shape=shape((own, width), BF16),
            grid_spec=pltpu.PrefetchScalarGridSpec(
                num_scalar_prefetch=1,
                grid=(steps,),
                in_specs=[
                    pl.BlockSpec((part_tile, vc), moving),
                    pl.BlockSpec((part_tile, wc), moving),
                    pl.BlockSpec((part_tile, gc), moving),
                    pl.BlockSpec((part_tile, pc), moving),
                    pl.BlockSpec((part_tile // BLOCK, heads, BLOCK), lambda i, off: (off[0] + i, 0, 0)),
                    pl.BlockSpec((vc, STATE), fixed),
                    pl.BlockSpec((1, vc), fixed),
                    pl.BlockSpec((vc, width), fixed),
                    pl.BlockSpec((pc, width), fixed),
                ],
                out_specs=pl.BlockSpec((part_tile, width), lambda i, off: (i, 0)),
            ),
            compiler_params=PARAMS,
            cost_estimate=cost(2 * own * width * (vc + pc), 4 * width * (own + vc)),
        )(
            jnp.reshape(member * steps, (1,)).astype(jnp.int32),
            y,
            reads,
            gate,
            branch,
            cumg,
            incoming,
            gated_norm_scale[None, :],
            state_output_matrix,
            pooling_output_matrix,
        )

    arrived = []
    for d in range(1, tp):
        sent = part(lax.rem(rank + d, tp))
        arrived.append(lax.ppermute(sent, "tp", [(i, (i + d) % tp) for i in range(tp)]))
    mixed = part(rank).astype(F32)
    for block in arrived:
        mixed = mixed + block.astype(F32)
    return mixed.astype(BF16)


def solution(mesh):
    placed = (
        P(("sp", "tp"), None),
        P(),
        P(None, "tp"),
        P(None, "tp"),
        P(None, "tp"),
        P(None, "tp"),
        P(),
        P(None, "tp"),
        P(None, "tp"),
        P(None, "tp"),
        P(None, "tp"),
        P(),
        P("tp", "sp"),
        P("tp", "sp"),
        P("tp"),
        P("tp", None, None),
        P("tp"),
        P("tp", None),
        P("tp", None),
    )
    return jax.shard_map(
        functools.partial(shards, mesh.shape["tp"], mesh.shape["sp"]),
        mesh=mesh,
        in_specs=placed,
        out_specs=P(("sp", "tp"), None),
        check_vma=False,
    )
```

```python
import functools

import jax
import jax.numpy as jnp
from jax import lax
from jax.experimental import pallas as pl
from jax.experimental.pallas import tpu as pltpu
from jax.sharding import PartitionSpec as P

HEAD_DIM = 64
STATE = 128
BLOCK = 128
POOL_DIM = 64
TAIL = 16
EPS = 1e-06
F32 = jnp.float32
BF16 = jnp.bfloat16
HIGHEST = lax.Precision.HIGHEST

VMEM = pl.BlockSpec(memory_space=pltpu.VMEM)
HBM = pl.BlockSpec(memory_space=pltpu.HBM)
PARAMS = pltpu.CompilerParams(vmem_limit_bytes=12 * 1024 * 1024)
SMALL = pltpu.CompilerParams(vmem_limit_bytes=4 * 1024 * 1024)


def iota(shape, axis):
    return lax.broadcasted_iota(jnp.int32, shape, axis)


def silu(v):
    half = 0.5 * v
    return half + half * jnp.tanh(half)


def rows_at(i, n):
    return pl.ds(pl.multiple_of(i * n, n), n)


def tdot(a, b):
    return lax.dot_general(a, b, (((1,), (1,)), ((), ())), preferred_element_type=F32)


def triple(v):
    high = v.astype(BF16).astype(F32)
    mid = (v - high).astype(BF16).astype(F32)
    return high, mid, v - high - mid


def spread(rows, width):
    heads = rows.shape[0]
    high, mid, low = triple(rows)
    split = jnp.concatenate([high, mid, low], axis=0).astype(BF16)
    wide = (3 * heads, heads * width)
    pick = (iota(wide, 1) // width == iota(wide, 0) % heads).astype(BF16)
    return lax.dot_general(split, pick, (((0,), (0,)), ((), ())), preferred_element_type=F32)


def norm_rows(x, scale):
    wide = x.astype(F32)
    mean = jnp.mean(wide * wide, axis=-1, keepdims=True)
    return (wide * lax.rsqrt(mean + EPS) * scale).astype(BF16)


def project(xn, i, tile, w):
    part = jnp.dot(xn[pl.ds(pl.multiple_of(TAIL + i * tile, TAIL), tile), :], w[...], preferred_element_type=F32)
    return part.astype(BF16).astype(F32)


def conv_matrix(xn, w, taps, out, ext, length, tile):
    cols = w.shape[1]
    reach = taps.shape[0] - 1
    ext[0:TAIL, 0:cols] = (
        jnp.dot(xn[0:TAIL, :], w[...], preferred_element_type=F32).astype(BF16).astype(F32)
    )

    @pl.loop(0, length // tile)
    def _(i):
        ext[TAIL : TAIL + tile, 0:cols] = project(xn, i, tile, w)
        total = taps[0:1, :] * ext[TAIL - reach : TAIL - reach + tile, 0:cols]
        for k in range(1, reach + 1):
            total = total + taps[k : k + 1, :] * ext[TAIL - reach + k : TAIL - reach + k + tile, 0:cols]
        out[rows_at(i, tile), :] = silu(total).astype(BF16)
        ext[0:TAIL, 0:cols] = ext[tile : tile + TAIL, 0:cols]


def kernel_a(tp, *refs):
    xs, halos = refs[:tp], refs[tp : 2 * tp]
    smalls = refs[2 * tp : 2 * tp + 7]
    wv, ww = refs[2 * tp + 7 : 2 * tp + 9]
    (xn, vals, writes, step_o, cum_o, cumg_o, entry, pack) = refs[2 * tp + 9 : 2 * tp + 17]
    xv, wvb, wwb, ext, steps, carried = refs[2 * tp + 17 : 2 * tp + 23]
    scale, ws, tv, tw, rate, bias, extra = refs[2 * tp + 23 : 2 * tp + 30]
    sems = refs[-1]
    own = xs[0].shape[0]
    length = own * tp
    rank = lax.axis_index("tp")
    pairs = [(smalls[0], scale), (xs[0], xv)]
    pairs += list(zip(smalls[1:], (ws, tv, tw, rate, bias, extra)))
    pairs += [(wv, wvb), (ww, wwb)]
    copies = [pltpu.make_async_copy(src, dst, sems.at[i]) for i, (src, dst) in enumerate(pairs)]
    for c in copies:
        c.start()
    copies[0].wait()
    halo = halos[0][...].astype(F32)
    for h in halos[1:]:
        halo = halo + h[...].astype(F32)
    xn[0:TAIL, :] = norm_rows(halo, scale[...])
    small = min(64, own)
    for d in range(tp):
        if d == 0:
            copies[1].wait()
        held = xv if d == 0 else xs[d]
        source = lax.rem(rank - d + tp, tp)

        @pl.loop(0, own // small)
        def _(i):
            at = pl.multiple_of(TAIL + source * own + i * small, TAIL)
            xn[pl.ds(at, small), :] = norm_rows(held[rows_at(i, small), :], scale[...])

    tile = min(256, length)
    heads = bias.shape[0]

    for c in copies[2:8]:
        c.wait()

    @pl.loop(0, length // tile)
    def _(i):
        s = tdot(xn[pl.ds(pl.multiple_of(TAIL + i * tile, TAIL), tile), :], ws[...])
        s = s.astype(BF16).astype(F32)
        for b in range(tile // BLOCK):
            steps[i * (tile // BLOCK) + b] = s[b * BLOCK : (b + 1) * BLOCK, :].T

    copies[8].wait()
    conv_matrix(xn, wvb, tv, vals, ext, length, tile)
    copies[9].wait()
    conv_matrix(xn, wwb, tw, writes, ext, length, tile)

    blocks = length // BLOCK
    upper = (iota((BLOCK, BLOCK), 0) <= iota((BLOCK, BLOCK), 1)).astype(F32)
    wide_rate = (heads, rate.shape[1])
    mine = iota(wide_rate, 1) == iota(wide_rate, 0) + rank * heads
    own_rate = jnp.exp(
        jnp.sum(jnp.where(mine, jnp.broadcast_to(rate[...], wide_rate), 0.0), axis=1, keepdims=True)
    )
    carried[...] = jnp.zeros_like(carried)
    groups = ww.shape[1] // STATE
    total = jnp.zeros((heads, BLOCK), F32)
    step_all, decay_all = [], []
    for k in range(blocks):
        cols = slice(k * BLOCK, (k + 1) * BLOCK)
        every = steps[k]
        mine = jnp.zeros((heads, BLOCK), F32)
        for t in range(tp):
            mine = mine + jnp.where(rank == t, every[t * heads : (t + 1) * heads, :], 0.0)
        pre = mine + bias[:, cols]
        step = jnp.maximum(pre, 0.0) + jnp.log1p(jnp.exp(-jnp.abs(pre)))
        step_all.append(step)
        decay_all.append(extra[:, cols] - own_rate * step)
    cum_all = jnp.dot(
        jnp.concatenate(decay_all, axis=0), upper, precision=HIGHEST, preferred_element_type=F32
    )
    for k in range(blocks):
        cols = slice(k * BLOCK, (k + 1) * BLOCK)
        step = step_all[k]
        cum = cum_all[k * heads : (k + 1) * heads, :]
        step_o[k] = step
        cum_o[k] = cum
        cumg_o[k] = cum + total
        last = jnp.broadcast_to(cum[:, BLOCK - 1 : BLOCK], (heads, BLOCK))
        weight = spread(jnp.exp(last - cum) * step, HEAD_DIM)
        weighted = (vals[cols, :].astype(F32) * weight).astype(BF16)
        grow = jnp.exp(last)
        total = total + last
        for g in range(groups):
            lanes = slice(g * STATE, (g + 1) * STATE)
            contrib = lax.dot_general(
                weighted[:, lanes],
                writes[cols, lanes],
                (((0,), (0,)), ((), ())),
                preferred_element_type=F32,
            )
            entry[k, lanes, :] = carried[lanes, :].astype(BF16)
            repeat = STATE // HEAD_DIM
            for j in range(repeat):
                h = g * repeat + j
                at = slice(h * HEAD_DIM, (h + 1) * HEAD_DIM)
                carried[at, :] = (
                    carried[at, :] * grow[h : h + 1, :] + contrib[j * HEAD_DIM : (j + 1) * HEAD_DIM, :]
                )
    write_pack(pack, carried[...], total)


def write_pack(pack, state, total):
    wide = state.shape[0]
    heads = total.shape[0]
    pack[0:wide, :] = state.astype(BF16)
    high, mid, low = triple(total)
    filler = jnp.zeros((pack.shape[0] - wide - 3 * heads, STATE), F32)
    pack[wide:, :] = jnp.concatenate([high, mid, low, filler], axis=0).astype(BF16)


def kernel_scan(heads, *refs):
    packs, out = refs[:-1], refs[-1]
    wide = heads * HEAD_DIM
    passed = jnp.zeros((heads, STATE), F32)
    state = jnp.zeros((wide, STATE), F32)
    for p in packs:
        factor = jnp.exp(passed)
        tall = jnp.concatenate(
            [jnp.broadcast_to(factor[h : h + 1, :], (HEAD_DIM, STATE)) for h in range(heads)], axis=0
        )
        state = state + p[0:wide, :].astype(F32) * tall
        rest = p[wide:, :].astype(F32)
        passed = passed + (
            rest[0:heads, :] + rest[heads : 2 * heads, :] + rest[2 * heads : 3 * heads, :]
        )
    write_pack(out, state, passed)


def kernel_b1(
    tp, xn, wr, wg, wp, tr, pgm, pscale, reads, gate, branch, ext, a2, a4, a8, a16
):
    rank = lax.axis_index("tp")
    position0 = lax.axis_index("sp")
    length = xn.shape[0] - TAIL
    tile = min(256, length)
    conv_matrix(xn, wr, tr, reads, ext, length, tile)

    @pl.loop(0, length // tile)
    def _(i):
        gate[rows_at(i, tile), :] = jnp.dot(
            xn[pl.ds(pl.multiple_of(TAIL + i * tile, TAIL), tile), :], wg[...], preferred_element_type=F32
        ).astype(BF16)

    cols = wp.shape[1]
    groups = cols // POOL_DIM
    ext[0:TAIL, 0:cols] = (
        jnp.dot(xn[0:TAIL, :], wp[...], preferred_element_type=F32).astype(BF16).astype(F32)
    )
    level = lax.rem(rank * groups + iota((1, cols), 1) // POOL_DIM, 4)
    window = jnp.where(level == 0, 2, jnp.where(level == 1, 4, jnp.where(level == 2, 8, 16)))
    n = tile + TAIL
    twice = (iota((POOL_DIM, 2 * POOL_DIM), 1) % POOL_DIM == iota((POOL_DIM, 2 * POOL_DIM), 0)).astype(BF16)
    pair = 2 * POOL_DIM
    same = iota((pair, pair), 0) // POOL_DIM == iota((pair, pair), 1) // POOL_DIM

    @pl.loop(0, length // tile)
    def _(i):
        p = project(xn, i, tile, wp)
        ext[TAIL:n, 0:cols] = p
        a2[0:n, :] = ext[0:n, 0:cols] + ext[1 : n + 1, 0:cols]
        a4[0:n, :] = a2[0:n, :] + a2[2 : n + 2, :]
        a8[0:n, :] = a4[0:n, :] + a4[4 : n + 4, :]
        a16[0:n, :] = a8[0:n, :] + a8[8 : n + 8, :]
        total = jnp.where(
            level == 0,
            a2[15 : 15 + tile, :],
            jnp.where(
                level == 1,
                a4[13 : 13 + tile, :],
                jnp.where(level == 2, a8[9 : 9 + tile, :], a16[1 : 1 + tile, :]),
            ),
        )
        reached = position0 * length + i * tile + iota((tile, 1), 0) + 1
        share = jnp.where(reached < window, 1.0 / reached.astype(F32), 1.0 / window.astype(F32))
        diff = (total * share - p).astype(BF16)
        for j in range(groups // 2):
            lanes = slice(j * pair, (j + 1) * pair)
            both = jnp.dot(pgm[lanes, :], twice, preferred_element_type=F32)
            block = jnp.where(same, both, 0.0).astype(BF16)
            mapped = jnp.dot(diff[:, lanes], block, preferred_element_type=F32)
            branch[rows_at(i, tile), lanes] = (mapped * pscale[:, lanes]).astype(BF16)
        ext[0:TAIL, 0:cols] = ext[tile : tile + TAIL, 0:cols]


def kernel_b2(reads, writes, vals, step_i, cum_i, entry, y):
    groups = writes.shape[1] // STATE
    repeat = STATE // HEAD_DIM
    causal = iota((BLOCK, BLOCK), 0) >= iota((BLOCK, BLOCK), 1)
    lane = iota((BLOCK, STATE), 1) // HEAD_DIM

    @pl.loop(0, step_i.shape[0])
    def _(k):
        step = step_i[k]
        cum = cum_i[k]
        at = rows_at(k, BLOCK)
        tall = spread(cum, BLOCK)
        grown = jnp.exp(spread(cum, HEAD_DIM))
        for g in range(groups):
            lanes = slice(g * STATE, (g + 1) * STATE)
            read = reads[at, lanes]
            affinity = tdot(read, writes[at, lanes])
            value = vals[at, lanes].astype(F32)
            total = tdot(read, entry[k, lanes, :]) * grown[:, lanes]
            for j in range(repeat):
                h = g * repeat + j
                gap = tall[:, h * BLOCK : (h + 1) * BLOCK] - cum[h : h + 1, :]
                within = (
                    affinity * jnp.exp(jnp.where(causal, gap, -jnp.inf)) * step[h : h + 1, :]
                ).astype(BF16)
                part = jnp.where(lane == j, value, 0.0).astype(BF16)
                total = total + jnp.dot(within, part, preferred_element_type=F32)
            y[at, lanes] = total


def kernel_c(tp, ahead, y, reads, gate, branch, cumg, incoming, gnorm, so, po, *rest):
    out = rest[-1]
    groups = y.shape[1] // STATE
    own = out.shape[0]
    member = lax.rem(lax.axis_index("tp") + ahead, tp)
    tile = min(256, own)

    @pl.loop(0, own // tile)
    def _(i):
        at = pl.ds(pl.multiple_of(member * own + i * tile, tile), tile)
        block = (member * own + i * tile) // BLOCK
        grown = jnp.concatenate(
            [jnp.exp(spread(cumg[block + b], HEAD_DIM)) for b in range(tile // BLOCK)], axis=0
        )
        pieces = []
        for g in range(groups):
            lanes = slice(g * STATE, (g + 1) * STATE)
            total = y[at, lanes] + grown[:, lanes] * tdot(reads[at, lanes], incoming[lanes, :])
            gated = total * silu(gate[at, lanes].astype(F32))
            mean = jnp.mean(gated * gated, axis=-1, keepdims=True)
            pieces.append((gated * lax.rsqrt(mean + EPS) * gnorm[:, lanes]).astype(BF16))
        part = jnp.dot(
            jnp.concatenate(pieces, axis=1), so[...], preferred_element_type=F32
        ) + jnp.dot(branch[at, :], po[...], preferred_element_type=F32)
        rounded = part.astype(BF16)
        if len(rest) > 1:
            total = rounded.astype(F32)
            for block_in in rest[:-1]:
                total = total + block_in[rows_at(i, tile), :].astype(F32)
            rounded = total.astype(BF16)
        out[rows_at(i, tile), :] = rounded


def pinned(v):
    return pltpu.with_memory_space_constraint(v, pltpu.HBM)


def shape(s, t):
    return jax.ShapeDtypeStruct(s, t)


def cost(flops, size):
    return pl.CostEstimate(flops=int(flops), bytes_accessed=int(size), transcendentals=0)


def shards(
    tp,
    sp,
    activations,
    input_norm_scale,
    value_weight_matrix,
    gate_weight_matrix,
    write_weight_matrix,
    read_weight_matrix,
    step_weight_matrix,
    pooling_input_matrix,
    value_filter_weight,
    write_filter_weight,
    read_filter_weight,
    head_log_decay_rate,
    step_bias_offset,
    position_log_decay,
    gated_norm_scale,
    pooling_group_matrix,
    pooling_channel_scale,
    state_output_matrix,
    pooling_output_matrix,
):
    own, width = activations.shape
    length = own * tp
    vc = value_weight_matrix.shape[1]
    wc = write_weight_matrix.shape[1]
    gc = gate_weight_matrix.shape[1]
    pc = pooling_input_matrix.shape[1]
    heads = vc // HEAD_DIM
    blocks = length // BLOCK
    every = step_weight_matrix.shape[1]
    tile = min(256, length)
    rank = lax.axis_index("tp")

    tail = activations[own - TAIL :, :]
    xs = [activations]
    for d in range(1, tp):
        xs.append(lax.ppermute(activations, "tp", [(i, (i + d) % tp) for i in range(tp)]))
    halos = [
        lax.ppermute(tail, ("sp", "tp"), [(s * tp - 1, s * tp + t) for s in range(1, sp)])
        for t in range(tp)
    ]
    pack_rows = -(-(vc + 3 * heads) // 16) * 16
    xn, vals, writes, step, cum, cumg, entry, pack = pl.pallas_call(
        functools.partial(kernel_a, tp),
        name="front",
        out_shape=(
            shape((TAIL + length, width), BF16),
            shape((length, vc), BF16),
            shape((length, wc), BF16),
            shape((blocks, heads, BLOCK), F32),
            shape((blocks, heads, BLOCK), F32),
            shape((blocks, heads, BLOCK), F32),
            shape((blocks, vc, STATE), BF16),
            shape((pack_rows, STATE), BF16),
        ),
        in_specs=[HBM] + [VMEM] * (2 * tp - 1) + [HBM] * 9,
        out_specs=[VMEM] * 8,
        scratch_shapes=[
            pltpu.VMEM((own, width), BF16),
            pltpu.VMEM((width, vc), BF16),
            pltpu.VMEM((width, wc), BF16),
            pltpu.VMEM((TAIL + tile, max(vc, wc)), F32),
            pltpu.VMEM((blocks, every, BLOCK), F32),
            pltpu.VMEM((vc, STATE), F32),
            pltpu.VMEM((1, width), F32),
            pltpu.VMEM((every, width), BF16),
            pltpu.VMEM(value_filter_weight.shape, F32),
            pltpu.VMEM(write_filter_weight.shape, F32),
            pltpu.VMEM((1, every), F32),
            pltpu.VMEM(step_bias_offset.shape, F32),
            pltpu.VMEM(position_log_decay.shape, F32),
            pltpu.SemaphoreType.DMA((10,)),
        ],
        compiler_params=PARAMS,
        cost_estimate=cost(2 * length * width * (vc + wc), 4 * width * (length + vc)),
    )(
        pinned(activations),
        *xs[1:],
        *halos,
        pinned(input_norm_scale[None, :]),
        pinned(step_weight_matrix.T),
        pinned(value_filter_weight),
        pinned(write_filter_weight),
        pinned(head_log_decay_rate[None, :]),
        pinned(step_bias_offset),
        pinned(position_log_decay),
        pinned(value_weight_matrix),
        pinned(write_weight_matrix),
    )

    def from_before(block, distance):
        return lax.ppermute(block, "sp", [(s - distance, s) for s in range(distance, sp)])

    def combine(packs):
        return pl.pallas_call(
            functools.partial(kernel_scan, heads),
            name="scan",
            out_shape=shape((pack_rows, STATE), BF16),
            in_specs=[VMEM] * len(packs),
            out_specs=VMEM,
            compiler_params=SMALL,
            cost_estimate=cost(vc * STATE * 8, vc * STATE * 8),
        )(*packs)

    first = [from_before(pack, d) for d in range(1, 5) if d < sp]

    tall = tile + TAIL + 16
    reads, gate, branch = pl.pallas_call(
        functools.partial(kernel_b1, tp),
        name="middle",
        out_shape=(shape((length, wc), BF16), shape((length, gc), BF16), shape((length, pc), BF16)),
        in_specs=[VMEM] * 7,
        out_specs=[VMEM] * 3,
        scratch_shapes=[
            pltpu.VMEM((tall, max(wc, pc)), F32),
            pltpu.VMEM((tall, pc), F32),
            pltpu.VMEM((tall, pc), F32),
            pltpu.VMEM((tall, pc), F32),
            pltpu.VMEM((tall, pc), F32),
        ],
        compiler_params=PARAMS,
        cost_estimate=cost(2 * length * width * (gc + wc + pc), 4 * width * (length + vc)),
    )(
        xn,
        read_weight_matrix,
        gate_weight_matrix,
        pooling_input_matrix,
        read_filter_weight,
        pooling_group_matrix.reshape(pc, POOL_DIM),
        pooling_channel_scale[None, :],
    )

    covered = combine(first)
    reach = 4
    second = []
    while reach < sp:
        parts = [covered] + [from_before(covered, d * reach) for d in range(1, 4) if d * reach < sp]
        second.append(parts)
        covered = combine(parts)
        reach *= 4
    incoming = covered

    y = pl.pallas_call(
        kernel_b2,
        name="inside",
        out_shape=shape((length, vc), F32),
        in_specs=[VMEM] * 6,
        out_specs=VMEM,
        compiler_params=PARAMS,
        cost_estimate=cost(8e9, 8 * length * vc),
    )(reads, writes, vals, step, cum, entry)

    def part(ahead, others):
        return pl.pallas_call(
            functools.partial(kernel_c, tp, ahead),
            name="back",
            out_shape=shape((own, width), BF16),
            in_specs=[VMEM] * (9 + len(others)),
            out_specs=VMEM,
            compiler_params=PARAMS,
            cost_estimate=cost(2 * own * width * (vc + pc), 4 * width * (own + vc)),
        )(
            y,
            reads,
            gate,
            branch,
            cumg,
            incoming,
            gated_norm_scale[None, :],
            state_output_matrix,
            pooling_output_matrix,
            *others,
        )

    arrived = []
    for d in range(1, tp):
        arrived.append(lax.ppermute(part(d, []), "tp", [(i, (i + d) % tp) for i in range(tp)]))
    return part(0, arrived)


def solution(mesh):
    placed = (
        P(("sp", "tp"), None),
        P(),
        P(None, "tp"),
        P(None, "tp"),
        P(None, "tp"),
        P(None, "tp"),
        P(),
        P(None, "tp"),
        P(None, "tp"),
        P(None, "tp"),
        P(None, "tp"),
        P(),
        P("tp", "sp"),
        P("tp", "sp"),
        P("tp"),
        P("tp", None, None),
        P("tp"),
        P("tp", None),
        P("tp", None),
    )
    return jax.shard_map(
        functools.partial(shards, mesh.shape["tp"], mesh.shape["sp"]),
        mesh=mesh,
        in_specs=placed,
        out_specs=P(("sp", "tp"), None),
        check_vma=False,
    )
```

```python
import functools

import jax
import jax.numpy as jnp
from jax import lax
from jax.experimental import pallas as pl
from jax.experimental.pallas import tpu as pltpu
from jax.sharding import PartitionSpec as P

HEAD_DIM = 64
STATE = 128
BLOCK = 128
POOL_DIM = 64
TAIL = 16
EPS = 1e-06
F32 = jnp.float32
BF16 = jnp.bfloat16
HIGHEST = lax.Precision.HIGHEST

VMEM = pl.BlockSpec(memory_space=pltpu.VMEM)
HBM = pl.BlockSpec(memory_space=pltpu.HBM)
PARAMS = pltpu.CompilerParams(vmem_limit_bytes=12 * 1024 * 1024)
SMALL = pltpu.CompilerParams(vmem_limit_bytes=4 * 1024 * 1024)


def iota(shape, axis):
    return lax.broadcasted_iota(jnp.int32, shape, axis)


def silu(v):
    half = 0.5 * v
    return half + half * jnp.tanh(half)


def rows_at(i, n):
    return pl.ds(pl.multiple_of(i * n, n), n)


def tdot(a, b):
    return lax.dot_general(a, b, (((1,), (1,)), ((), ())), preferred_element_type=F32)


def triple(v):
    high = v.astype(BF16).astype(F32)
    mid = (v - high).astype(BF16).astype(F32)
    return high, mid, v - high - mid


def spread(rows, width):
    heads = rows.shape[0]
    high, mid, low = triple(rows)
    split = jnp.concatenate([high, mid, low], axis=0).astype(BF16)
    wide = (3 * heads, heads * width)
    pick = (iota(wide, 1) // width == iota(wide, 0) % heads).astype(BF16)
    return lax.dot_general(split, pick, (((0,), (0,)), ((), ())), preferred_element_type=F32)


def norm_rows(x, scale):
    wide = x.astype(F32)
    mean = jnp.mean(wide * wide, axis=-1, keepdims=True)
    return (wide * lax.rsqrt(mean + EPS) * scale).astype(BF16)


def project(xn, i, tile, w):
    part = jnp.dot(xn[pl.ds(pl.multiple_of(TAIL + i * tile, TAIL), tile), :], w[...], preferred_element_type=F32)
    return part.astype(BF16).astype(F32)


def conv_matrix(xn, w, taps, out, ext, length, tile):
    cols = w.shape[1]
    reach = taps.shape[0] - 1
    ext[0, 0:TAIL, 0:cols] = (
        jnp.dot(xn[0:TAIL, :], w[...], preferred_element_type=F32).astype(BF16).astype(F32)
    )
    for i in range(length // tile):
        at = i % 2
        ext[at, TAIL : TAIL + tile, 0:cols] = project(xn, i, tile, w)
        ext[1 - at, 0:TAIL, 0:cols] = ext[at, tile : tile + TAIL, 0:cols]
        total = taps[0:1, :] * ext[at, TAIL - reach : TAIL - reach + tile, 0:cols]
        for k in range(1, reach + 1):
            total = total + taps[k : k + 1, :] * ext[at, TAIL - reach + k : TAIL - reach + k + tile, 0:cols]
        out[i * tile : (i + 1) * tile, :] = silu(total).astype(BF16)


def kernel_a(tp, *refs):
    xs, halos = refs[:tp], refs[tp : 2 * tp]
    smalls = refs[2 * tp : 2 * tp + 7]
    wv, ww = refs[2 * tp + 7 : 2 * tp + 9]
    (xn, vals, writes, step_o, cum_o, cumg_o, entry, pack) = refs[2 * tp + 9 : 2 * tp + 17]
    xv, wvb, wwb, ext, steps, carried = refs[2 * tp + 17 : 2 * tp + 23]
    scale, ws, tv, tw, rate, bias, extra = refs[2 * tp + 23 : 2 * tp + 30]
    sems = refs[-1]
    own = xs[0].shape[0]
    length = own * tp
    rank = lax.axis_index("tp")
    pairs = [(smalls[0], scale), (xs[0], xv)]
    pairs += list(zip(smalls[1:], (ws, tv, tw, rate, bias, extra)))
    pairs += [(wv, wvb), (ww, wwb)]
    copies = [pltpu.make_async_copy(src, dst, sems.at[i]) for i, (src, dst) in enumerate(pairs)]
    for c in copies:
        c.start()
    copies[0].wait()
    halo = halos[0][...].astype(F32)
    for h in halos[1:]:
        halo = halo + h[...].astype(F32)
    xn[0:TAIL, :] = norm_rows(halo, scale[...])
    small = min(64, own)
    for d in range(tp):
        if d == 0:
            copies[1].wait()
        held = xv if d == 0 else xs[d]
        source = lax.rem(rank - d + tp, tp)

        @pl.loop(0, own // small)
        def _(i):
            at = pl.multiple_of(TAIL + source * own + i * small, TAIL)
            xn[pl.ds(at, small), :] = norm_rows(held[rows_at(i, small), :], scale[...])

    tile = min(256, length)
    heads = bias.shape[0]

    for c in copies[2:8]:
        c.wait()

    @pl.loop(0, length // tile)
    def _(i):
        s = tdot(xn[pl.ds(pl.multiple_of(TAIL + i * tile, TAIL), tile), :], ws[...])
        s = s.astype(BF16).astype(F32)
        for b in range(tile // BLOCK):
            steps[i * (tile // BLOCK) + b] = s[b * BLOCK : (b + 1) * BLOCK, :].T

    copies[8].wait()
    conv_matrix(xn, wvb, tv, vals, ext, length, tile)
    copies[9].wait()
    conv_matrix(xn, wwb, tw, writes, ext, length, tile)

    blocks = length // BLOCK
    upper = (iota((BLOCK, BLOCK), 0) <= iota((BLOCK, BLOCK), 1)).astype(F32)
    wide_rate = (heads, rate.shape[1])
    mine = iota(wide_rate, 1) == iota(wide_rate, 0) + rank * heads
    own_rate = jnp.exp(
        jnp.sum(jnp.where(mine, jnp.broadcast_to(rate[...], wide_rate), 0.0), axis=1, keepdims=True)
    )
    carried[...] = jnp.zeros_like(carried)
    groups = ww.shape[1] // STATE
    total = jnp.zeros((heads, BLOCK), F32)
    step_all, decay_all = [], []
    for k in range(blocks):
        cols = slice(k * BLOCK, (k + 1) * BLOCK)
        every = steps[k]
        mine = jnp.zeros((heads, BLOCK), F32)
        for t in range(tp):
            mine = mine + jnp.where(rank == t, every[t * heads : (t + 1) * heads, :], 0.0)
        pre = mine + bias[:, cols]
        step = jnp.maximum(pre, 0.0) + jnp.log1p(jnp.exp(-jnp.abs(pre)))
        step_all.append(step)
        decay_all.append(extra[:, cols] - own_rate * step)
    cum_all = jnp.dot(
        jnp.concatenate(decay_all, axis=0), upper, precision=HIGHEST, preferred_element_type=F32
    )
    for k in range(blocks):
        cols = slice(k * BLOCK, (k + 1) * BLOCK)
        step = step_all[k]
        cum = cum_all[k * heads : (k + 1) * heads, :]
        step_o[k] = step
        cum_o[k] = cum
        cumg_o[k] = cum + total
        last = jnp.broadcast_to(cum[:, BLOCK - 1 : BLOCK], (heads, BLOCK))
        weight = spread(jnp.exp(last - cum) * step, HEAD_DIM)
        weighted = (vals[cols, :].astype(F32) * weight).astype(BF16)
        grow = jnp.exp(last)
        total = total + last
        for g in range(groups):
            lanes = slice(g * STATE, (g + 1) * STATE)
            contrib = lax.dot_general(
                weighted[:, lanes],
                writes[cols, lanes],
                (((0,), (0,)), ((), ())),
                preferred_element_type=F32,
            )
            entry[k, lanes, :] = carried[lanes, :].astype(BF16)
            repeat = STATE // HEAD_DIM
            for j in range(repeat):
                h = g * repeat + j
                at = slice(h * HEAD_DIM, (h + 1) * HEAD_DIM)
                carried[at, :] = (
                    carried[at, :] * grow[h : h + 1, :] + contrib[j * HEAD_DIM : (j + 1) * HEAD_DIM, :]
                )
    write_pack(pack, carried[...], total)


def write_pack(pack, state, total):
    wide = state.shape[0]
    heads = total.shape[0]
    pack[0:wide, :] = state.astype(BF16)
    high, mid, low = triple(total)
    filler = jnp.zeros((pack.shape[0] - wide - 3 * heads, STATE), F32)
    pack[wide:, :] = jnp.concatenate([high, mid, low, filler], axis=0).astype(BF16)


def kernel_scan(heads, *refs):
    packs, out = refs[:-1], refs[-1]
    wide = heads * HEAD_DIM
    passed = jnp.zeros((heads, STATE), F32)
    state = jnp.zeros((wide, STATE), F32)
    for p in packs:
        factor = jnp.exp(passed)
        tall = jnp.concatenate(
            [jnp.broadcast_to(factor[h : h + 1, :], (HEAD_DIM, STATE)) for h in range(heads)], axis=0
        )
        state = state + p[0:wide, :].astype(F32) * tall
        rest = p[wide:, :].astype(F32)
        passed = passed + (
            rest[0:heads, :] + rest[heads : 2 * heads, :] + rest[2 * heads : 3 * heads, :]
        )
    write_pack(out, state, passed)


def kernel_b1(xn, wr, wg, tr, reads, gate, ext):
    length = xn.shape[0] - TAIL
    tile = min(256, length)
    conv_matrix(xn, wr, tr, reads, ext, length, tile)

    @pl.loop(0, length // tile)
    def _(i):
        gate[rows_at(i, tile), :] = jnp.dot(
            xn[pl.ds(pl.multiple_of(TAIL + i * tile, TAIL), tile), :], wg[...], preferred_element_type=F32
        ).astype(BF16)


def kernel_pool(xn, wp, pgm, pscale, branch, exts, a2, a4, a8, a16):
    rank = lax.axis_index("tp")
    position0 = lax.axis_index("sp")
    length = xn.shape[0] - TAIL
    tile = min(256, length)
    cols = wp.shape[1]
    groups = cols // POOL_DIM
    exts[0, 0:TAIL, :] = (
        jnp.dot(xn[0:TAIL, :], wp[...], preferred_element_type=F32).astype(BF16).astype(F32)
    )
    level = lax.rem(rank * groups + iota((1, cols), 1) // POOL_DIM, 4)
    window = jnp.where(level == 0, 2, jnp.where(level == 1, 4, jnp.where(level == 2, 8, 16)))
    n = tile + TAIL
    twice = (iota((POOL_DIM, 2 * POOL_DIM), 1) % POOL_DIM == iota((POOL_DIM, 2 * POOL_DIM), 0)).astype(BF16)
    pair = 2 * POOL_DIM
    same = iota((pair, pair), 0) // POOL_DIM == iota((pair, pair), 1) // POOL_DIM
    mapped_by = []
    for j in range(groups // 2):
        both = jnp.dot(pgm[j * pair : (j + 1) * pair, :], twice, preferred_element_type=F32)
        mapped_by.append(jnp.where(same, both, 0.0).astype(BF16))

    for i in range(length // tile):
        p = project(xn, i, tile, wp)
        ext = exts.at[i % 2]
        ext[TAIL:n, :] = p
        exts[1 - i % 2, 0:TAIL, :] = ext[tile : tile + TAIL, :]
        a2[0:n, :] = ext[0:n, :] + ext[1 : n + 1, :]
        a4[0:n, :] = a2[0:n, :] + a2[2 : n + 2, :]
        a8[0:n, :] = a4[0:n, :] + a4[4 : n + 4, :]
        a16[0:n, :] = a8[0:n, :] + a8[8 : n + 8, :]
        total = jnp.where(
            level == 0,
            a2[15 : 15 + tile, :],
            jnp.where(
                level == 1,
                a4[13 : 13 + tile, :],
                jnp.where(level == 2, a8[9 : 9 + tile, :], a16[1 : 1 + tile, :]),
            ),
        )
        reached = position0 * length + i * tile + iota((tile, 1), 0) + 1
        share = jnp.where(reached < window, 1.0 / reached.astype(F32), 1.0 / window.astype(F32))
        diff = (total * share - ext[TAIL:n, :]).astype(BF16)
        for j in range(groups // 2):
            lanes = slice(j * pair, (j + 1) * pair)
            mapped = jnp.dot(diff[:, lanes], mapped_by[j], preferred_element_type=F32)
            branch[i * tile : (i + 1) * tile, lanes] = (mapped * pscale[:, lanes]).astype(BF16)


def kernel_b2(reads, writes, vals, step_i, cum_i, entry, y):
    groups = writes.shape[1] // STATE
    repeat = STATE // HEAD_DIM
    causal = iota((BLOCK, BLOCK), 0) >= iota((BLOCK, BLOCK), 1)
    lane = iota((BLOCK, STATE), 1) // HEAD_DIM

    @pl.loop(0, step_i.shape[0])
    def _(k):
        step = step_i[k]
        cum = cum_i[k]
        at = rows_at(k, BLOCK)
        tall = spread(cum, BLOCK)
        grown = jnp.exp(spread(cum, HEAD_DIM))
        for g in range(groups):
            lanes = slice(g * STATE, (g + 1) * STATE)
            read = reads[at, lanes]
            affinity = tdot(read, writes[at, lanes])
            value = vals[at, lanes].astype(F32)
            total = tdot(read, entry[k, lanes, :]) * grown[:, lanes]
            for j in range(repeat):
                h = g * repeat + j
                gap = tall[:, h * BLOCK : (h + 1) * BLOCK] - cum[h : h + 1, :]
                within = (
                    affinity * jnp.exp(jnp.where(causal, gap, -jnp.inf)) * step[h : h + 1, :]
                ).astype(BF16)
                part = jnp.where(lane == j, value, 0.0).astype(BF16)
                total = total + jnp.dot(within, part, preferred_element_type=F32)
            y[at, lanes] = total


def kernel_c(tp, ahead, y, reads, gate, branch, cumg, incoming, gnorm, so, po, out):
    groups = y.shape[1] // STATE
    own = out.shape[0]
    member = lax.rem(lax.axis_index("tp") + ahead, tp)
    tile = min(256, own)

    @pl.loop(0, own // tile)
    def _(i):
        at = pl.ds(pl.multiple_of(member * own + i * tile, tile), tile)
        block = (member * own + i * tile) // BLOCK
        grown = jnp.concatenate(
            [jnp.exp(spread(cumg[block + b], HEAD_DIM)) for b in range(tile // BLOCK)], axis=0
        )
        pieces = []
        for g in range(groups):
            lanes = slice(g * STATE, (g + 1) * STATE)
            total = y[at, lanes] + grown[:, lanes] * tdot(reads[at, lanes], incoming[lanes, :])
            gated = total * silu(gate[at, lanes].astype(F32))
            mean = jnp.mean(gated * gated, axis=-1, keepdims=True)
            pieces.append((gated * lax.rsqrt(mean + EPS) * gnorm[:, lanes]).astype(BF16))
        part = jnp.dot(
            jnp.concatenate(pieces, axis=1), so[...], preferred_element_type=F32
        ) + jnp.dot(branch[at, :], po[...], preferred_element_type=F32)
        rounded = part.astype(BF16)
        out[rows_at(i, tile), :] = rounded


def pinned(v):
    return pltpu.with_memory_space_constraint(v, pltpu.HBM)


def shape(s, t):
    return jax.ShapeDtypeStruct(s, t)


def cost(flops, size):
    return pl.CostEstimate(flops=int(flops), bytes_accessed=int(size), transcendentals=0)


def shards(
    tp,
    sp,
    activations,
    input_norm_scale,
    value_weight_matrix,
    gate_weight_matrix,
    write_weight_matrix,
    read_weight_matrix,
    step_weight_matrix,
    pooling_input_matrix,
    value_filter_weight,
    write_filter_weight,
    read_filter_weight,
    head_log_decay_rate,
    step_bias_offset,
    position_log_decay,
    gated_norm_scale,
    pooling_group_matrix,
    pooling_channel_scale,
    state_output_matrix,
    pooling_output_matrix,
):
    own, width = activations.shape
    length = own * tp
    vc = value_weight_matrix.shape[1]
    wc = write_weight_matrix.shape[1]
    gc = gate_weight_matrix.shape[1]
    pc = pooling_input_matrix.shape[1]
    heads = vc // HEAD_DIM
    blocks = length // BLOCK
    every = step_weight_matrix.shape[1]
    tile = min(256, length)
    rank = lax.axis_index("tp")

    tail = activations[own - TAIL :, :]
    xs = [activations]
    for d in range(1, tp):
        xs.append(lax.ppermute(activations, "tp", [(i, (i + d) % tp) for i in range(tp)]))
    halos = [
        lax.ppermute(tail, ("sp", "tp"), [(s * tp - 1, s * tp + t) for s in range(1, sp)])
        for t in range(tp)
    ]
    pack_rows = -(-(vc + 3 * heads) // 16) * 16
    xn, vals, writes, step, cum, cumg, entry, pack = pl.pallas_call(
        functools.partial(kernel_a, tp),
        name="front",
        out_shape=(
            shape((TAIL + length, width), BF16),
            shape((length, vc), BF16),
            shape((length, wc), BF16),
            shape((blocks, heads, BLOCK), F32),
            shape((blocks, heads, BLOCK), F32),
            shape((blocks, heads, BLOCK), F32),
            shape((blocks, vc, STATE), BF16),
            shape((pack_rows, STATE), BF16),
        ),
        in_specs=[HBM] + [VMEM] * (2 * tp - 1) + [HBM] * 9,
        out_specs=[VMEM] * 8,
        scratch_shapes=[
            pltpu.VMEM((own, width), BF16),
            pltpu.VMEM((width, vc), BF16),
            pltpu.VMEM((width, wc), BF16),
            pltpu.VMEM((2, TAIL + tile, max(vc, wc)), F32),
            pltpu.VMEM((blocks, every, BLOCK), F32),
            pltpu.VMEM((vc, STATE), F32),
            pltpu.VMEM((1, width), F32),
            pltpu.VMEM((every, width), BF16),
            pltpu.VMEM(value_filter_weight.shape, F32),
            pltpu.VMEM(write_filter_weight.shape, F32),
            pltpu.VMEM((1, every), F32),
            pltpu.VMEM(step_bias_offset.shape, F32),
            pltpu.VMEM(position_log_decay.shape, F32),
            pltpu.SemaphoreType.DMA((10,)),
        ],
        compiler_params=PARAMS,
        cost_estimate=cost(2 * length * width * (vc + wc), 4 * width * (length + vc)),
    )(
        pinned(activations),
        *xs[1:],
        *halos,
        pinned(input_norm_scale[None, :]),
        pinned(step_weight_matrix.T),
        pinned(value_filter_weight),
        pinned(write_filter_weight),
        pinned(head_log_decay_rate[None, :]),
        pinned(step_bias_offset),
        pinned(position_log_decay),
        pinned(value_weight_matrix),
        pinned(write_weight_matrix),
    )

    def from_before(block, distance):
        return lax.ppermute(block, "sp", [(s - distance, s) for s in range(distance, sp)])

    def combine(packs):
        return pl.pallas_call(
            functools.partial(kernel_scan, heads),
            name="scan",
            out_shape=shape((pack_rows, STATE), BF16),
            in_specs=[VMEM] * len(packs),
            out_specs=VMEM,
            compiler_params=SMALL,
            cost_estimate=cost(vc * STATE * 8, vc * STATE * 8),
        )(*packs)

    first = [from_before(pack, d) for d in range(1, 5) if d < sp]

    tall = tile + TAIL + 16
    reads, gate = pl.pallas_call(
        kernel_b1,
        name="middle",
        out_shape=(shape((length, wc), BF16), shape((length, gc), BF16)),
        in_specs=[VMEM] * 4,
        out_specs=[VMEM] * 2,
        scratch_shapes=[pltpu.VMEM((2, TAIL + tile, wc), F32)],
        compiler_params=PARAMS,
        cost_estimate=cost(2 * length * width * (gc + wc), 4 * width * (length + vc)),
    )(xn, read_weight_matrix, gate_weight_matrix, read_filter_weight)

    covered = combine(first)
    xn, reads, covered = lax.optimization_barrier((xn, reads, covered))
    reach = 4
    second = []
    while reach < sp:
        parts = [covered] + [from_before(covered, d * reach) for d in range(1, 4) if d * reach < sp]
        second.append(parts)
        covered = combine(parts)
        reach *= 4
    incoming = covered

    branch = pl.pallas_call(
        kernel_pool,
        name="pool",
        out_shape=shape((length, pc), BF16),
        in_specs=[VMEM] * 4,
        out_specs=VMEM,
        scratch_shapes=[pltpu.VMEM((2, tall, pc), F32)] + [pltpu.VMEM((tall, pc), F32)] * 4,
        compiler_params=PARAMS,
        cost_estimate=cost(2 * length * width * pc, 2 * width * (length + pc)),
    )(
        xn,
        pooling_input_matrix,
        pooling_group_matrix.reshape(pc, POOL_DIM),
        pooling_channel_scale[None, :],
    )

    y = pl.pallas_call(
        kernel_b2,
        name="inside",
        out_shape=shape((length, vc), F32),
        in_specs=[VMEM] * 6,
        out_specs=VMEM,
        compiler_params=PARAMS,
        cost_estimate=cost(8e9, 8 * length * vc),
    )(reads, writes, vals, step, cum, entry)

    def part(ahead):
        return pl.pallas_call(
            functools.partial(kernel_c, tp, ahead),
            name="back",
            out_shape=shape((own, width), BF16),
            in_specs=[VMEM] * 9,
            out_specs=VMEM,
            compiler_params=PARAMS,
            cost_estimate=cost(2 * own * width * (vc + pc), 4 * width * (own + vc)),
        )(
            y,
            reads,
            gate,
            branch,
            cumg,
            incoming,
            gated_norm_scale[None, :],
            state_output_matrix,
            pooling_output_matrix,
        )

    arrived = []
    for d in range(1, tp):
        arrived.append(lax.ppermute(part(d), "tp", [(i, (i + d) % tp) for i in range(tp)]))
    mixed = part(0).astype(F32)
    for block in arrived:
        mixed = mixed + block.astype(F32)
    return mixed.astype(BF16)


def solution(mesh):
    placed = (
        P(("sp", "tp"), None),
        P(),
        P(None, "tp"),
        P(None, "tp"),
        P(None, "tp"),
        P(None, "tp"),
        P(),
        P(None, "tp"),
        P(None, "tp"),
        P(None, "tp"),
        P(None, "tp"),
        P(),
        P("tp", "sp"),
        P("tp", "sp"),
        P("tp"),
        P("tp", None, None),
        P("tp"),
        P("tp", None),
        P("tp", None),
    )
    return jax.shard_map(
        functools.partial(shards, mesh.shape["tp"], mesh.shape["sp"]),
        mesh=mesh,
        in_specs=placed,
        out_specs=P(("sp", "tp"), None),
        check_vma=False,
    )
```
